32 devices in a mesh: sp: 8 (over z, y), tp: 4 (over x, core).
Axes of the slice: x: 2, y: 2, z: 4, core: 2. Of those that a mesh axis runs over, the one named last changes fastest.
Arguments:
- residual_in: bfloat16 [4096, 2048], P('sp'), may hold values from -6 to 6
- queries_nope: bfloat16 [4096, 1024], P('sp', 'tp'), may hold values from -15 to 15
- queries_rope: bfloat16 [4096, 512], P('sp', 'tp'), may hold values from -400 to 400
- latents: bfloat16 [4096, 256], P('sp'), may hold values from -6 to 6
- rope_keys: bfloat16 [4096, 32], P('sp'), may hold values from -8 to 8
- latent_norm_gain: float32 [256], replicated, may hold values from 0.1 to 1.9
- key_up_weight: bfloat16 [256, 1024], P(None, 'tp'), may hold values from -0.375 to 0.375
- value_up_weight: bfloat16 [256, 1024], P(None, 'tp'), may hold values from -0.375 to 0.375
- w_out: bfloat16 [1024, 2048], P('tp'), may hold values from -0.59765625 to 0.59765625
- norm_gain: float32 [2048], replicated, may hold values from 0.1 to 1.9
- w_up: bfloat16 [2048, 8192], P('sp', 'tp'), may hold values from -0.125 to 0.125
- w_down: bfloat16 [8192, 2048], P('tp', 'sp'), may hold values from -0.0625 to 0.0625
Outputs:
- layer_out: bfloat16 [4096, 2048], P('sp', 'tp')
The draws below stay inside these ranges and needn't reach their ends.
All inputs are finite; a program needn't handle non-finite values.
Results may differ from the reference program's by a relative error of at most 0.015.
Values may be sent and summed in bfloat16 or wider, within the bound.
A program may use at most 128 MiB of HBM per device.

```python
import math
import jax
import jax.numpy as jnp
from jax import lax

D = 2048
HEAD_TOTAL = 16
UNROTATED_WIDTH = 64
ROPE = 32
VALUE_WIDTH = 64
LATENT_WIDTH = 256
FF = 8192
TOKEN_TOTAL = 4096
N_TP = 4


def shared_rope(key):
    base_rows = jnp.clip(jax.random.normal(jax.random.fold_in(key, 11), (TOKEN_TOTAL, ROPE), jnp.float32), -4.0, 4.0)
    return base_rows


def draw_rope_keys(key, part):
    base_rows = shared_rope(key)
    return base_rows.astype(jnp.bfloat16)


def draw_queries_rope(key, part):
    drawn = jnp.clip(jax.random.normal(jax.random.fold_in(key, 21), (TOKEN_TOTAL, HEAD_TOTAL * ROPE), jnp.float32) * 2.5, -15.0, 15.0)
    return drawn.astype(jnp.bfloat16)


def level_of(stream_key, dims, shards, least, largest):
    factor_of, own = 1.0, jax.random.fold_in(stream_key, 6)
    for axis_at, blocks in shards:
        draws = jnp.exp(jax.random.uniform(jax.random.fold_in(own, axis_at), (blocks,), jnp.float32, least / len(shards), largest / len(shards)))
        factor_of = factor_of * jnp.repeat(draws, dims[axis_at] // blocks).reshape([-1 if axis == axis_at else 1 for axis in range(len(dims))])
    return factor_of


def bell_draw(own_key, extent, scale, reach, pieces=(), kind=jnp.bfloat16):
    gain = level_of(own_key, extent, pieces, -0.22, 0.18) if pieces else 1.0
    entries = jax.random.normal(own_key, extent, jnp.float32) * scale * gain
    return jnp.minimum(jnp.maximum(entries, -reach), reach).astype(kind)


def setup_inputs(seed: int = 0) -> dict:
    keys = jax.random.split(jax.random.key(seed), 13)
    residual_in = bell_draw(keys[0], (TOKEN_TOTAL, D), 1.0, 6.0, ((0, 8),))
    queries_nope = bell_draw(keys[1], (TOKEN_TOTAL, HEAD_TOTAL * UNROTATED_WIDTH), 2.5, 15.0, ((0, 8), (1, 4)))
    queries_rope = draw_queries_rope(jax.random.fold_in(keys[12], 71), 0)
    latents = bell_draw(keys[3], (TOKEN_TOTAL, LATENT_WIDTH), 1.0, 6.0, ((0, 8),))
    rope_keys = draw_rope_keys(jax.random.fold_in(keys[12], 71), 0)
    latent_norm_gain = jnp.clip(1.0 + 0.18 * jax.random.normal(keys[5], (LATENT_WIDTH,), jnp.float32), 0.1, 1.9)
    key_up_weight = bell_draw(keys[6], (LATENT_WIDTH, HEAD_TOTAL * UNROTATED_WIDTH), LATENT_WIDTH ** -0.5, 0.375, ((1, 4),))
    value_up_weight = bell_draw(keys[7], (LATENT_WIDTH, HEAD_TOTAL * VALUE_WIDTH), LATENT_WIDTH ** -0.5, 0.375, ((1, 4),))
    w_out = bell_draw(keys[8], (HEAD_TOTAL * VALUE_WIDTH, D), 0.1, 0.59765625, ((0, 4),))
    norm_gain = jnp.clip(1.0 + 0.18 * jax.random.normal(keys[9], (D,), jnp.float32), 0.1, 1.9)
    w_up = bell_draw(keys[10], (D, FF), D ** -0.5, 0.125, ((0, 8), (1, 4)))
    w_down = bell_draw(keys[11], (FF, D), FF ** -0.5, 0.0625, ((0, 4), (1, 8)))
    return dict(residual_in=residual_in, queries_nope=queries_nope, queries_rope=queries_rope, latents=latents, rope_keys=rope_keys, latent_norm_gain=latent_norm_gain, key_up_weight=key_up_weight, value_up_weight=value_up_weight, w_out=w_out, norm_gain=norm_gain, w_up=w_up, w_down=w_down)


rope_base = 10000.0
epsilon = 1e-06

def rotate(vectors, phases):
    half_width = vectors.shape[-1] // 2
    first_half = vectors[..., :half_width]
    second_half = vectors[..., half_width:]
    cosine = jnp.cos(phases)
    sine = jnp.sin(phases)
    return jnp.concatenate([first_half * cosine - second_half * sine, second_half * cosine + first_half * sine], axis=-1)

def rope_phases(positions, width):
    inverse = 1.0 / rope_base ** (jnp.arange(0, width, 2, dtype=jnp.float32) / width)
    return positions.astype(jnp.float32)[:, None] * inverse[None, :]

def rms_scale(vectors, gain_vec):
    return vectors * lax.rsqrt(lax.optimization_barrier(jnp.mean(vectors * vectors, axis=-1, keepdims=True)) + epsilon) * gain_vec.astype(jnp.float32)

def reference(residual_in, queries_nope, queries_rope, latents, rope_keys, latent_norm_gain, key_up_weight, value_up_weight, w_out, norm_gain, w_up, w_down):
    positions = jnp.arange(TOKEN_TOTAL, dtype=jnp.int32)
    phases = rope_phases(positions, ROPE)
    q_rot = rotate(queries_rope.astype(jnp.float32).reshape(TOKEN_TOTAL, HEAD_TOTAL, ROPE), phases[:, None, :]).astype(jnp.bfloat16)
    queries = jnp.concatenate([queries_nope.reshape(TOKEN_TOTAL, HEAD_TOTAL, UNROTATED_WIDTH), q_rot], axis=2)
    lat_norm = rms_scale(latents.astype(jnp.float32), latent_norm_gain).astype(jnp.bfloat16)
    key_nope = jnp.dot(lat_norm, key_up_weight, preferred_element_type=jnp.float32).astype(jnp.bfloat16).reshape(TOKEN_TOTAL, HEAD_TOTAL, UNROTATED_WIDTH)
    values = jnp.dot(lat_norm, value_up_weight, preferred_element_type=jnp.float32).astype(jnp.bfloat16).reshape(TOKEN_TOTAL, HEAD_TOTAL, VALUE_WIDTH)
    key_rot = rotate(rope_keys.astype(jnp.float32), phases).astype(jnp.bfloat16)
    key_all = jnp.concatenate([key_nope, jnp.broadcast_to(key_rot[:, None, :], (TOKEN_TOTAL, HEAD_TOTAL, ROPE))], axis=2).astype(jnp.float32)
    value_all = values.astype(jnp.float32)
    score_scale = 1.0 / math.sqrt(UNROTATED_WIDTH + ROPE)
    query_rows = math.gcd(TOKEN_TOTAL, 128)

    def attend(query_block):
        scores = jnp.einsum('qhd,khd->hqk', query_block.astype(jnp.float32), key_all) * score_scale
        row_peak = lax.optimization_barrier(jnp.max(scores, axis=2, keepdims=True))
        weights = jnp.exp(scores - row_peak)
        denominator = lax.optimization_barrier(jnp.sum(weights, axis=2))
        rounded = lax.optimization_barrier(weights.astype(jnp.bfloat16)).astype(jnp.float32)
        weighted = jnp.einsum('hqk,khd->qhd', rounded, value_all)
        return (weighted / jnp.transpose(denominator)[:, :, None]).astype(jnp.bfloat16)
    attended = lax.map(attend, queries.reshape(TOKEN_TOTAL // query_rows, query_rows, HEAD_TOTAL, UNROTATED_WIDTH + ROPE))
    attended = attended.reshape(TOKEN_TOTAL, HEAD_TOTAL * VALUE_WIDTH)
    group_cols = HEAD_TOTAL * VALUE_WIDTH // N_TP
    summed = jnp.zeros((TOKEN_TOTAL, D), jnp.float32)
    for member in range(N_TP):
        part_term = jnp.dot(attended[:, member * group_cols:(member + 1) * group_cols], w_out[member * group_cols:(member + 1) * group_cols], preferred_element_type=jnp.float32)
        summed = summed + lax.optimization_barrier(part_term.astype(jnp.bfloat16)).astype(jnp.float32)
    stream = residual_in.astype(jnp.float32) + summed
    normed = rms_scale(stream, norm_gain).astype(jnp.bfloat16)
    upward = jnp.dot(normed, w_up, preferred_element_type=jnp.float32)
    hidden = jnp.square(jax.nn.relu(upward)).astype(jnp.bfloat16)
    group_units = FF // N_TP
    mixer = jnp.zeros((TOKEN_TOTAL, D), jnp.float32)
    for member in range(N_TP):
        part_term = jnp.dot(hidden[:, member * group_units:(member + 1) * group_units], w_down[member * group_units:(member + 1) * group_units], preferred_element_type=jnp.float32)
        mixer = mixer + lax.optimization_barrier(part_term.astype(jnp.bfloat16)).astype(jnp.float32)
    return (stream + mixer).astype(jnp.bfloat16)
```

```python
import functools
import math

import jax
import jax.numpy as jnp
from jax import lax
from jax.experimental import pallas as pl
from jax.experimental.pallas import tpu as pltpu
from jax.sharding import PartitionSpec as P

UNROTATED_WIDTH = 64
ROPE = 32
LANES = 128

rope_base = 10000.0
epsilon = 1e-06
F32 = jnp.float32
BF16 = jnp.bfloat16
MESH = pl.DeviceIdType.MESH
NT = (((1,), (1,)), ((), ()))


def rotate(vectors, phases):
    half_width = vectors.shape[-1] // 2
    first_half = vectors[..., :half_width]
    second_half = vectors[..., half_width:]
    cosine = jnp.cos(phases)
    sine = jnp.sin(phases)
    return jnp.concatenate(
        [first_half * cosine - second_half * sine, second_half * cosine + first_half * sine],
        axis=-1,
    )


def rope_phases(positions, width):
    inverse = 1.0 / rope_base ** (jnp.arange(0, width, 2, dtype=jnp.float32) / width)
    return positions.astype(jnp.float32)[:, None] * inverse[None, :]


def rms_scale(vectors, gain_vec):
    return (
        vectors
        * lax.rsqrt(jnp.mean(vectors * vectors, axis=-1, keepdims=True) + epsilon)
        * gain_vec
    )


def ring_of(index, n):
    return index // 2 + (index % 2) * (n - 1 - 2 * (index // 2))


def index_of(place, n):
    return 2 * place + (place // (n // 2)) * (2 * n - 1 - 4 * place)


def ring_ids(n):
    place = ring_of(lax.axis_index("sp"), n)

    def at(offset):
        return index_of((place + offset + 2 * n) % n, n)

    return at


def attention_kernel(
    n, heads, scale, q_ref, x_ref, wk_ref, wv_ref, wo_ref, wu_ref,
    part_ref, full_ref,
    xs, peak, acc, xsend, xrecv, wsend, wrecv, own_sem,
):
    at = ring_ids(n)
    tp = lax.axis_index("tp")
    me = lax.axis_index("sp")
    to = ((at(1), tp), (at(-1), tp))
    barrier = pltpu.get_barrier_semaphore()
    for target in to:
        pl.semaphore_signal(barrier, inc=1, device_id=target, device_id_type=MESH)
    pl.semaphore_wait(barrier, 2)

    latent = wk_ref.shape[1]
    value_width = wv_ref.shape[0] // heads

    def x_copy(step, half, src):
        return pltpu.make_async_remote_copy(
            src_ref=src, dst_ref=xs.at[step + 1, half],
            send_sem=xsend.at[step, half], recv_sem=xrecv.at[step, half],
            device_id=to[half], device_id_type=MESH,
        )

    def w_copy(step, half, src):
        owner = at(-step) if half == 0 else at(step)
        return pltpu.make_async_remote_copy(
            src_ref=full_ref.at[owner, half] if src is None else src,
            dst_ref=full_ref.at[owner, half],
            send_sem=wsend.at[step, half], recv_sem=wrecv.at[step, half],
            device_id=to[half], device_id_type=MESH,
        )

    for half in range(2):
        x_copy(0, half, x_ref.at[half]).start()
    for half in range(2):
        w_copy(0, half, wu_ref.at[half]).start()
    own = pltpu.make_async_copy(wu_ref, full_ref.at[me], own_sem)
    own.start()
    peak[...] = jnp.full(peak.shape, -1e30, F32)
    acc[...] = jnp.zeros(acc.shape, F32)

    def attend(block_a, block_b):
        block = jnp.concatenate([block_a, block_b], axis=1)
        lat = block[:latent]
        rot = block[latent:]
        keys = block.shape[1]
        k_all = jnp.dot(wk_ref[...], lat, preferred_element_type=F32).astype(BF16)
        v_all = jnp.dot(wv_ref[...], lat, preferred_element_type=F32).astype(BF16)
        k_pad = jnp.zeros((LANES - UNROTATED_WIDTH - rot.shape[0], keys), BF16)
        ones = jnp.ones((16, keys), BF16)
        v_pad = jnp.zeros((LANES - value_width - 16, keys), BF16)
        for h in range(heads):
            k_h = jnp.concatenate(
                [k_all[h * UNROTATED_WIDTH:(h + 1) * UNROTATED_WIDTH], rot, k_pad], axis=0)
            v_h = jnp.concatenate(
                [v_all[h * value_width:(h + 1) * value_width], ones, v_pad], axis=0)
            s = jnp.dot(q_ref[:, h * LANES:(h + 1) * LANES], k_h, preferred_element_type=F32)
            old = peak[h]
            new = jnp.maximum(old, jnp.max(s, axis=1, keepdims=True))
            p = jnp.exp2((s - new) * scale).astype(BF16)
            acc[h] = acc[h] * jnp.exp2((old - new) * scale) + lax.dot_general(
                p, v_h, NT, preferred_element_type=F32)
            peak[h] = new

    attend(x_ref[0], x_ref[1])

    def turn(i, carry):
        for half in range(2):
            x_copy(i - 1, half, x_ref.at[half]).wait_recv()

            @pl.when(i < n - 1)
            def _():
                x_copy(i, half, xs.at[i, half]).start()

        for half in range(2):
            w_copy(i - 1, half, wu_ref.at[half]).wait_recv()

            @pl.when(i < n - 1)
            def _():
                w_copy(i, half, None).start()

        attend(xs[i, 0], xs[i, 1])
        return carry

    lax.fori_loop(1, n, turn, 0)

    width = part_ref.shape[2]
    group = []
    for h in range(heads):
        a = acc[h]
        group.append((a[:, :value_width] / a[:, value_width:value_width + 1]).astype(BF16))
    attended = jnp.concatenate(group, axis=1)
    for j in range(part_ref.shape[0]):
        part_ref[j] = jnp.dot(
            attended, wo_ref[:, j * width:(j + 1) * width], preferred_element_type=F32
        ).astype(BF16)

    own.wait()

    def drain(i, carry):
        for half in range(2):
            x_copy(i, half, x_ref.at[half]).wait_send()
            w_copy(i, half, wu_ref.at[half]).wait_send()
        return carry

    lax.fori_loop(0, n - 1, drain, 0)


def feed_kernel(
    n, n_tp, narrow, part_ref, res_ref, gain_ref, up_hbm, wd_ref,
    out_ref,
    up, down, parts, ys, sq, own_stream, hidden, pieces, fin,
    dsend, drecv, psend, precv, ysend, yrecv, qsend, qrecv, fsend, frecv, local,
):
    at = ring_ids(n)
    tp = lax.axis_index("tp")
    sp = lax.axis_index("sp")
    to = ((at(1), tp), (at(-1), tp))
    peers = [(tp + k) % n_tp for k in range(1, n_tp)]
    barrier = pltpu.get_barrier_semaphore()
    for target in list(to) + [(sp, p) for p in peers]:
        pl.semaphore_signal(barrier, inc=1, device_id=target, device_id_type=MESH)
    pl.semaphore_wait(barrier, 2 + n_tp - 1)

    rows, width = res_ref.shape
    per = n // n_tp

    def d_copy(step, half, src):
        return pltpu.make_async_remote_copy(
            src_ref=down.at[step, half] if src is None else src,
            dst_ref=down.at[step + 1, half],
            send_sem=dsend.at[step, half], recv_sem=drecv.at[step, half],
            device_id=to[half], device_id_type=MESH,
        )

    def p_copy(k):
        peer = peers[k]
        return pltpu.make_async_remote_copy(
            src_ref=part_ref.at[peer], dst_ref=parts.at[k],
            send_sem=psend.at[k], recv_sem=precv.at[k],
            device_id=(sp, peer), device_id_type=MESH,
        )

    def y_copy(k):
        return pltpu.make_async_remote_copy(
            src_ref=ys.at[tp], dst_ref=ys.at[tp],
            send_sem=ysend.at[k], recv_sem=yrecv.at[k],
            device_id=(sp, peers[k]), device_id_type=MESH,
        )

    def q_copy(k):
        return pltpu.make_async_remote_copy(
            src_ref=sq.at[0], dst_ref=sq.at[k + 1],
            send_sem=qsend.at[k], recv_sem=qrecv.at[k],
            device_id=(sp, peers[k]), device_id_type=MESH,
        )

    def event(step):
        for half in range(2):
            d_copy(step - 1, half, wd_ref.at[half]).wait_recv()
            d_copy(step, half, None).start()

    for half in range(2):
        d_copy(0, half, wd_ref.at[half]).start()
    for k in range(n_tp - 1):
        p_copy(k).start()
    load = pltpu.make_async_copy(up_hbm, up, local.at[0])
    load.start()
    early = min(n - 2, 5)

    def maybe(step):
        if step <= early:
            event(step)

    maybe(1)
    for k in range(n_tp - 1):
        p_copy(k).wait_recv()
    maybe(2)
    stream = part_ref[tp].astype(F32)
    for k in range(n_tp - 1):
        stream = stream + parts[k].astype(F32)
    stream = stream + res_ref[...].astype(F32)
    own_stream[...] = stream
    ys[tp] = (stream * gain_ref[...]).astype(BF16)
    total = jnp.sum(stream * stream, axis=1, keepdims=True)
    sq[0] = jnp.transpose(jnp.broadcast_to(total, (rows, LANES)))[:8]
    for k in range(n_tp - 1):
        q_copy(k).start()
        y_copy(k).start()
    maybe(3)
    for k in range(n_tp - 1):
        q_copy(k).wait_recv()
    for k in range(n_tp - 1):
        pltpu.make_async_remote_copy(
            src_ref=ys.at[tp], dst_ref=ys.at[(tp + n_tp - 1 - k) % n_tp],
            send_sem=ysend.at[k], recv_sem=yrecv.at[k],
            device_id=(sp, peers[k]), device_id_type=MESH,
        ).wait_recv()
    maybe(4)
    squares = sq[0]
    for k in range(1, n_tp):
        squares = squares + sq[k]
    squares = jnp.concatenate([squares] * (LANES // 8), axis=0)
    factor = lax.rsqrt(jnp.transpose(squares)[:, :1] / (width * n_tp) + epsilon)
    load.wait()
    units = hidden.shape[1]
    tile = math.gcd(units, 512)

    def up_step(c, carry):
        columns = pl.ds(pl.multiple_of(c * tile, tile), tile)
        total = jnp.dot(ys[0], up[:width, columns], preferred_element_type=F32)
        for t in range(1, n_tp):
            total = total + jnp.dot(
                ys[t], up[t * width:(t + 1) * width, columns], preferred_element_type=F32)
        total = jnp.maximum(total, 0.0) * factor
        hidden[:, columns] = (total * total).astype(BF16)
        return carry

    lax.fori_loop(0, units // tile, up_step, 0)
    maybe(5)

    def owners(i):
        return at(-i), at(i)

    def f_copy(i, half, owner):
        return pltpu.make_async_remote_copy(
            src_ref=pieces.at[i, half],
            dst_ref=fin.at[tp, owner % per, half],
            send_sem=fsend.at[i, half], recv_sem=frecv.at[tp, owner % per, half],
            device_id=(sp, owner // per), device_id_type=MESH,
        )

    def down_block(i, left, right):
        if narrow:
            block = jnp.concatenate([left, right], axis=0)
            half_width = left.shape[0]
            term = lax.dot_general(hidden[...], block, NT, preferred_element_type=F32)
        else:
            block = jnp.concatenate([left, right], axis=1)
            half_width = left.shape[1]
            term = jnp.dot(hidden[...], block, preferred_element_type=F32)
        term = term.astype(BF16)
        pieces[i, 0] = term[:, :half_width]
        pieces[i, 1] = term[:, half_width:]
        for half, owner in enumerate(owners(i)):

            @pl.when(owner // per != tp)
            def _():
                f_copy(i, half, owner).start()

            @pl.when(owner // per == tp)
            def _():
                fin[tp, owner % per, half] = pieces[i, half]

    down_block(0, wd_ref[0], wd_ref[1])

    def down_step(i, carry):
        @pl.when(i > early)
        def _():
            for half in range(2):
                d_copy(i - 1, half, wd_ref.at[half]).wait_recv()

        @pl.when(jnp.logical_and(i > early, i < n - 1))
        def _():
            for half in range(2):
                d_copy(i, half, None).start()

        down_block(i, down[i, 0], down[i, 1])
        return carry

    lax.fori_loop(1, n, down_step, 0)

    for k in range(n_tp - 1):
        source = (tp + n_tp - 1 - k) % n_tp
        for o in range(per):
            for half in range(2):
                pltpu.make_async_remote_copy(
                    src_ref=pieces.at[0, half], dst_ref=fin.at[source, o, half],
                    send_sem=fsend.at[0, half], recv_sem=frecv.at[source, o, half],
                    device_id=(sp, peers[k]), device_id_type=MESH,
                ).wait_recv()
    piece = fin.shape[4]
    for o in range(per):
        for half in range(2):
            start = (2 * o + half) * piece
            total = own_stream[:, start:start + piece]
            mixed = fin[0, o, half].astype(F32)
            for t in range(1, n_tp):
                mixed = mixed + fin[t, o, half].astype(F32)
            out_ref[:, start:start + piece] = (total + mixed).astype(BF16)

    def drain(i, carry):
        for half in range(2):
            d_copy(i, half, wd_ref.at[half]).wait_send()
        return carry

    lax.fori_loop(0, n - 1, drain, 0)

    def drain_pieces(i, carry):
        for half, owner in enumerate(owners(i)):

            @pl.when(owner // per != tp)
            def _():
                f_copy(i, half, owner).wait_send()

        return carry

    lax.fori_loop(0, n, drain_pieces, 0)
    for k in range(n_tp - 1):
        p_copy(k).wait_send()
        q_copy(k).wait_send()
        y_copy(k).wait_send()


def vmem():
    return pl.BlockSpec(memory_space=pltpu.VMEM)


def hbm():
    return pl.BlockSpec(memory_space=pl.ANY)


def on_device(
    n,
    n_tp,
    residual_in,
    queries_nope,
    queries_rope,
    latents,
    rope_keys,
    latent_norm_gain,
    key_up_weight,
    value_up_weight,
    w_out,
    norm_gain,
    w_up,
    w_down,
):
    rows, model = residual_in.shape
    heads = key_up_weight.shape[1] // UNROTATED_WIDTH
    value_width = value_up_weight.shape[1] // heads
    positions = lax.axis_index("sp") * rows + jnp.arange(rows, dtype=jnp.int32)
    phases = rope_phases(positions, ROPE)
    q_rot = rotate(
        queries_rope.astype(F32).reshape(rows, heads, ROPE), phases[:, None, :]
    ).astype(BF16)
    queries = jnp.concatenate(
        [
            queries_nope.reshape(rows, heads, UNROTATED_WIDTH),
            q_rot,
            jnp.zeros((rows, heads, LANES - UNROTATED_WIDTH - ROPE), BF16),
        ],
        axis=2,
    ).reshape(rows, heads * LANES)
    lat_norm = rms_scale(latents.astype(F32), latent_norm_gain).astype(BF16)
    key_rot = rotate(rope_keys.astype(F32), phases).astype(BF16)
    x = jnp.concatenate([lat_norm, key_rot], axis=1)
    wide = x.shape[1]
    x = jnp.transpose(x.reshape(2, rows // 2, wide), (0, 2, 1))

    width = model // n_tp
    depth, units = w_up.shape
    dma = pltpu.SemaphoreType.DMA
    part, full = pl.pallas_call(
        functools.partial(
            attention_kernel, n, heads,
            math.log2(math.e) / math.sqrt(UNROTATED_WIDTH + ROPE)),
        out_shape=(
            jax.ShapeDtypeStruct((n_tp, rows, width), BF16),
            jax.ShapeDtypeStruct((n, 2, depth // 2, units), BF16),
        ),
        in_specs=[vmem()] * 5 + [hbm()],
        out_specs=(vmem(), hbm()),
        scratch_shapes=[
            pltpu.VMEM((n, 2, wide, rows // 2), BF16),
            pltpu.VMEM((heads, rows, 1), F32),
            pltpu.VMEM((heads, rows, LANES), F32),
            dma((n - 1, 2)), dma((n - 1, 2)), dma((n - 1, 2)), dma((n - 1, 2)), dma,
        ],
        compiler_params=pltpu.CompilerParams(
            collective_id=0, has_side_effects=True, vmem_limit_bytes=56 * 2**20),
        name="attend",
    )(
        queries, x, jnp.transpose(key_up_weight), jnp.transpose(value_up_weight),
        w_out, w_up.reshape(2, depth // 2, units),
    )

    hidden_units, share = w_down.shape
    narrow = (share // 2) % LANES != 0
    halves = jnp.transpose(
        w_down.reshape(hidden_units, 2, share // 2), (1, 2, 0) if narrow else (1, 0, 2))
    t = lax.axis_index("tp")
    own_residual = lax.dynamic_slice_in_dim(residual_in, t * width, width, 1)
    own_gain = lax.dynamic_slice_in_dim(norm_gain, t * width, width, 0)[None, :]
    per = n // n_tp
    return pl.pallas_call(
        functools.partial(feed_kernel, n, n_tp, narrow),
        out_shape=jax.ShapeDtypeStruct((rows, width), BF16),
        in_specs=[vmem()] * 3 + [hbm(), vmem()],
        out_specs=vmem(),
        scratch_shapes=[
            pltpu.VMEM((model, units), BF16),
            pltpu.VMEM((n,) + halves.shape, BF16),
            pltpu.VMEM((n_tp - 1, rows, width), BF16),
            pltpu.VMEM((n_tp, rows, width), BF16),
            pltpu.VMEM((n_tp, 8, rows), F32),
            pltpu.VMEM((rows, width), F32),
            pltpu.VMEM((rows, units), BF16),
            pltpu.VMEM((n, 2, rows, share // 2), BF16),
            pltpu.VMEM((n_tp, per, 2, rows, share // 2), BF16),
            dma((n - 1, 2)), dma((n - 1, 2)),
            dma((n_tp - 1,)), dma((n_tp - 1,)),
            dma((n_tp - 1,)), dma((n_tp - 1,)),
            dma((n_tp - 1,)), dma((n_tp - 1,)),
            dma((n, 2)), dma((n_tp, per, 2)),
            dma((1,)),
        ],
        compiler_params=pltpu.CompilerParams(
            collective_id=1, has_side_effects=True, vmem_limit_bytes=60 * 2**20),
        name="feed",
    )(part, own_residual, own_gain, full.reshape(model, units), halves)


def solution(mesh):
    in_specs = (
        P("sp", None),
        P("sp", "tp"),
        P("sp", "tp"),
        P("sp", None),
        P("sp", None),
        P(),
        P(None, "tp"),
        P(None, "tp"),
        P("tp", None),
        P(),
        P("sp", "tp"),
        P("tp", "sp"),
    )
    out_specs = P("sp", "tp")
    return jax.shard_map(
        functools.partial(on_device, mesh.shape["sp"], mesh.shape["tp"]),
        mesh=mesh, in_specs=in_specs, out_specs=out_specs, check_vma=False,
    )
```

```python
import functools
import math

import jax
import jax.numpy as jnp
from jax import lax
from jax.experimental import pallas as pl
from jax.experimental.pallas import tpu as pltpu
from jax.sharding import PartitionSpec as P

UNROTATED_WIDTH = 64
ROPE = 32
LANES = 128
CHUNKS = 4

rope_base = 10000.0
epsilon = 1e-06
F32 = jnp.float32
BF16 = jnp.bfloat16
MESH = pl.DeviceIdType.MESH
NT = (((1,), (1,)), ((), ()))


def rotate(vectors, phases):
    half_width = vectors.shape[-1] // 2
    first_half = vectors[..., :half_width]
    second_half = vectors[..., half_width:]
    cosine = jnp.cos(phases)
    sine = jnp.sin(phases)
    return jnp.concatenate(
        [first_half * cosine - second_half * sine, second_half * cosine + first_half * sine],
        axis=-1,
    )


def rope_phases(positions, width):
    inverse = 1.0 / rope_base ** (jnp.arange(0, width, 2, dtype=jnp.float32) / width)
    return positions.astype(jnp.float32)[:, None] * inverse[None, :]


def rms_scale(vectors, gain_vec):
    return (
        vectors
        * lax.rsqrt(jnp.mean(vectors * vectors, axis=-1, keepdims=True) + epsilon)
        * gain_vec
    )


def ring_of(index, n):
    return index // 2 + (index % 2) * (n - 1 - 2 * (index // 2))


def index_of(place, n):
    return 2 * place + (place // (n // 2)) * (2 * n - 1 - 4 * place)


def ring_ids(n):
    place = ring_of(lax.axis_index("sp"), n)

    def at(offset):
        return index_of((place + offset + 2 * n) % n, n)

    return at


def attention_kernel(
    n, n_tp, heads, scale, q_ref, x_ref, wk_ref, wv_ref, wo_ref, wu_ref,
    part_ref, full_ref,
    xs, peak, acc, xsend, xrecv, ssend, srecv, wsend, wrecv, own_sem,
):
    at = ring_ids(n)
    tp = lax.axis_index("tp")
    me = lax.axis_index("sp")
    to = ((at(1), tp), (at(-1), tp))
    peers = [(tp + k) % n_tp for k in range(1, n_tp)]
    onward = (at(1 - 2 * (tp % 2)), tp)
    barrier = pltpu.get_barrier_semaphore()
    for target in list(to) + [(me, p) for p in peers]:
        pl.semaphore_signal(barrier, inc=1, device_id=target, device_id_type=MESH)
    pl.semaphore_wait(barrier, 2 + n_tp - 1)

    latent = wk_ref.shape[1]
    value_width = wv_ref.shape[0] // heads

    def x_copy(step, src):
        return pltpu.make_async_remote_copy(
            src_ref=src, dst_ref=xs.at[step + 1, tp],
            send_sem=xsend.at[step], recv_sem=xrecv.at[step],
            device_id=onward, device_id_type=MESH,
        )

    def share(step, k):
        return pltpu.make_async_remote_copy(
            src_ref=xs.at[step, tp], dst_ref=xs.at[step, tp],
            send_sem=ssend.at[step, k], recv_sem=srecv.at[step, k],
            device_id=(me, peers[k]), device_id_type=MESH,
        )

    def share_wait(step):
        for k in range(n_tp - 1):
            pltpu.make_async_remote_copy(
                src_ref=xs.at[step, tp], dst_ref=xs.at[step, (tp + n_tp - 1 - k) % n_tp],
                send_sem=ssend.at[step, k], recv_sem=srecv.at[step, k],
                device_id=(me, peers[k]), device_id_type=MESH,
            ).wait_recv()

    def w_copy(step, half, c, first):
        owner = at(-step) if half == 0 else at(step)
        return pltpu.make_async_remote_copy(
            src_ref=wu_ref.at[half, c] if first else full_ref.at[owner, half, c],
            dst_ref=full_ref.at[owner, half, c],
            send_sem=wsend.at[step, half, c], recv_sem=wrecv.at[step, half, c],
            device_id=to[half], device_id_type=MESH,
        )

    x_copy(0, x_ref.at[tp]).start()
    for c in range(CHUNKS):
        for half in range(2):
            w_copy(0, half, c, True).start()
    own = pltpu.make_async_copy(wu_ref, full_ref.at[me], own_sem)
    own.start()
    peak[...] = jnp.full(peak.shape, -1e30, F32)
    acc[...] = jnp.zeros(acc.shape, F32)

    def attend(blocks):
        block = jnp.concatenate(blocks, axis=1)
        lat = block[:latent]
        rot = block[latent:]
        keys = block.shape[1]
        k_all = jnp.dot(wk_ref[...], lat, preferred_element_type=F32).astype(BF16)
        v_all = jnp.dot(wv_ref[...], lat, preferred_element_type=F32).astype(BF16)
        k_pad = jnp.zeros((LANES - UNROTATED_WIDTH - rot.shape[0], keys), BF16)
        ones = jnp.ones((16, keys), BF16)
        v_pad = jnp.zeros((LANES - value_width - 16, keys), BF16)
        for h in range(heads):
            k_h = jnp.concatenate(
                [k_all[h * UNROTATED_WIDTH:(h + 1) * UNROTATED_WIDTH], rot, k_pad], axis=0)
            v_h = jnp.concatenate(
                [v_all[h * value_width:(h + 1) * value_width], ones, v_pad], axis=0)
            s = jnp.dot(q_ref[:, h * LANES:(h + 1) * LANES], k_h, preferred_element_type=F32)
            old = peak[h]
            new = jnp.maximum(old, jnp.max(s, axis=1, keepdims=True))
            p = jnp.exp2((s - new) * scale).astype(BF16)
            acc[h] = acc[h] * jnp.exp2((old - new) * scale) + lax.dot_general(
                p, v_h, NT, preferred_element_type=F32)
            peak[h] = new

    def turn(i, carry):
        x_copy(i - 1, x_ref.at[tp]).wait_recv()

        @pl.when(i < n - 1)
        def _():
            x_copy(i, xs.at[i, tp]).start()

        for k in range(n_tp - 1):
            share(i, k).start()
        for c in range(CHUNKS):
            for half in range(2):
                w_copy(i - 1, half, c, True).wait_recv()

                @pl.when(i < n - 1)
                def _():
                    w_copy(i, half, c, False).start()

        @pl.when(i > 1)
        def _():
            share_wait(i - 1)
            attend([xs[i - 1, t] for t in range(n_tp)])

        return carry

    attend([x_ref[t] for t in range(n_tp)])
    lax.fori_loop(1, n, turn, 0)
    share_wait(n - 1)
    attend([xs[n - 1, t] for t in range(n_tp)])

    width = part_ref.shape[2]
    group = []
    for h in range(heads):
        a = acc[h]
        group.append((a[:, :value_width] / a[:, value_width:value_width + 1]).astype(BF16))
    attended = jnp.concatenate(group, axis=1)
    for j in range(part_ref.shape[0]):
        part_ref[j] = jnp.dot(
            attended, wo_ref[:, j * width:(j + 1) * width], preferred_element_type=F32
        ).astype(BF16)

    own.wait()

    def drain(i, carry):
        x_copy(i, x_ref.at[tp]).wait_send()
        for k in range(n_tp - 1):
            share(i + 1, k).wait_send()
        for c in range(CHUNKS):
            for half in range(2):
                w_copy(i, half, c, True).wait_send()
        return carry

    lax.fori_loop(0, n - 1, drain, 0)


def feed_kernel(
    n, n_tp, narrow, part_ref, res_hbm, gain_ref, up_hbm, wd_hbm,
    out_ref,
    res_ref, up, down, parts, ys, sq, own_stream, hidden, pieces, fin,
    dsend, drecv, psend, precv, ysend, yrecv, qsend, qrecv, fsend, frecv, local,
):
    at = ring_ids(n)
    tp = lax.axis_index("tp")
    sp = lax.axis_index("sp")
    to = ((at(1), tp), (at(-1), tp))
    peers = [(tp + k) % n_tp for k in range(1, n_tp)]
    barrier = pltpu.get_barrier_semaphore()
    for target in list(to) + [(sp, p) for p in peers]:
        pl.semaphore_signal(barrier, inc=1, device_id=target, device_id_type=MESH)
    pl.semaphore_wait(barrier, 2 + n_tp - 1)

    rows, width = res_ref.shape
    per = n // n_tp

    lines = down.shape[2] // CHUNKS

    def own_half(half):
        if narrow:
            return wd_hbm.at[half]
        return wd_hbm.at[:, half * down.shape[3]:(half + 1) * down.shape[3]]

    def d_copy(step, half, c, first):
        span = pl.ds(c * lines, lines)
        if not first:
            src = down.at[step, half, span]
        elif narrow:
            src = wd_hbm.at[half, span]
        else:
            src = wd_hbm.at[span, half * down.shape[3]:(half + 1) * down.shape[3]]
        return pltpu.make_async_remote_copy(
            src_ref=src, dst_ref=down.at[step + 1, half, span],
            send_sem=dsend.at[step, half, c], recv_sem=drecv.at[step, half, c],
            device_id=to[half], device_id_type=MESH,
        )

    def p_copy(k):
        peer = peers[k]
        return pltpu.make_async_remote_copy(
            src_ref=part_ref.at[peer], dst_ref=parts.at[k],
            send_sem=psend.at[k], recv_sem=precv.at[k],
            device_id=(sp, peer), device_id_type=MESH,
        )

    def y_copy(k):
        return pltpu.make_async_remote_copy(
            src_ref=ys.at[tp], dst_ref=ys.at[tp],
            send_sem=ysend.at[k], recv_sem=yrecv.at[k],
            device_id=(sp, peers[k]), device_id_type=MESH,
        )

    def q_copy(k):
        return pltpu.make_async_remote_copy(
            src_ref=sq.at[0], dst_ref=sq.at[k + 1],
            send_sem=qsend.at[k], recv_sem=qrecv.at[k],
            device_id=(sp, peers[k]), device_id_type=MESH,
        )

    def landed(step, c):
        for half in range(2):
            d_copy(step, half, c, True).wait_recv()

    def event(step, c):
        landed(step - 1, c)
        for half in range(2):
            d_copy(step, half, c, False).start()

    def events(first, last):
        for tick in range(first, last):
            event(1 + tick // CHUNKS, tick % CHUNKS)

    for c in range(CHUNKS):
        for half in range(2):
            d_copy(0, half, c, True).start()
    for k in range(n_tp - 1):
        p_copy(k).start()
    loads = [
        pltpu.make_async_copy(
            res_hbm.at[:, pl.ds(pl.multiple_of(tp * width, LANES), width)], res_ref, local.at[0]),
        pltpu.make_async_copy(up_hbm, up, local.at[1]),
        pltpu.make_async_copy(own_half(0), down.at[0, 0], local.at[2]),
        pltpu.make_async_copy(own_half(1), down.at[0, 1], local.at[3]),
    ]
    for load in loads:
        load.start()

    early = 4
    events(0, 6)
    for k in range(n_tp - 1):
        p_copy(k).wait_recv()
    loads[0].wait()
    stream = part_ref[tp].astype(F32)
    for k in range(n_tp - 1):
        stream = stream + parts[k].astype(F32)
    stream = stream + res_ref[...].astype(F32)
    own_stream[...] = stream
    ys[tp] = (stream * gain_ref[tp]).astype(BF16)
    total = jnp.sum(stream * stream, axis=1, keepdims=True)
    sq[0] = jnp.transpose(jnp.broadcast_to(total, (rows, LANES)))[:8]
    for k in range(n_tp - 1):
        q_copy(k).start()
        y_copy(k).start()
    events(6, 12)
    for k in range(n_tp - 1):
        q_copy(k).wait_recv()
    for k in range(n_tp - 1):
        pltpu.make_async_remote_copy(
            src_ref=ys.at[tp], dst_ref=ys.at[(tp + n_tp - 1 - k) % n_tp],
            send_sem=ysend.at[k], recv_sem=yrecv.at[k],
            device_id=(sp, peers[k]), device_id_type=MESH,
        ).wait_recv()
    squares = sq[0]
    for k in range(1, n_tp):
        squares = squares + sq[k]
    squares = jnp.concatenate([squares] * (LANES // 8), axis=0)
    factor = lax.rsqrt(jnp.transpose(squares)[:, :1] / (width * n_tp) + epsilon)
    loads[1].wait()
    units = hidden.shape[1]
    tile = math.gcd(units, 512)

    def up_step(c, carry):
        columns = pl.ds(pl.multiple_of(c * tile, tile), tile)
        total = jnp.dot(ys[0], up[:width, columns], preferred_element_type=F32)
        for t in range(1, n_tp):
            total = total + jnp.dot(
                ys[t], up[t * width:(t + 1) * width, columns], preferred_element_type=F32)
        total = jnp.maximum(total, 0.0) * factor
        hidden[:, columns] = (total * total).astype(BF16)

        @pl.when(c < CHUNKS)
        def _():
            event(early, c)

        return carry

    lax.fori_loop(0, units // tile, up_step, 0)

    def owners(i):
        return at(-i), at(i)

    def f_copy(i, half, owner):
        return pltpu.make_async_remote_copy(
            src_ref=pieces.at[i, half],
            dst_ref=fin.at[tp, owner % per, half],
            send_sem=fsend.at[i, half], recv_sem=frecv.at[tp, owner % per, half],
            device_id=(sp, owner // per), device_id_type=MESH,
        )

    def down_block(i, left, right):
        if narrow:
            block = jnp.concatenate([left, right], axis=0)
            half_width = left.shape[0]
            term = lax.dot_general(hidden[...], block, NT, preferred_element_type=F32)
        else:
            block = jnp.concatenate([left, right], axis=1)
            half_width = left.shape[1]
            term = jnp.dot(hidden[...], block, preferred_element_type=F32)
        term = term.astype(BF16)
        pieces[i, 0] = term[:, :half_width]
        pieces[i, 1] = term[:, half_width:]
        for half, owner in enumerate(owners(i)):

            @pl.when(owner // per != tp)
            def _():
                f_copy(i, half, owner).start()

            @pl.when(owner // per == tp)
            def _():
                fin[tp, owner % per, half] = pieces[i, half]

    for load in loads[2:]:
        load.wait()
    down_block(0, down[0, 0], down[0, 1])

    def down_step(i, carry):
        @pl.when(i <= CHUNKS)
        def _():
            event(early + 1, i - 1)

        @pl.when(i > early + 1)
        def _():
            for c in range(CHUNKS):
                landed(i - 1, c)

                @pl.when(i < n - 1)
                def _():
                    for half in range(2):
                        d_copy(i, half, c, False).start()

        down_block(i, down[i, 0], down[i, 1])
        return carry

    lax.fori_loop(1, n, down_step, 0)

    for k in range(n_tp - 1):
        source = (tp + n_tp - 1 - k) % n_tp
        for o in range(per):
            for half in range(2):
                pltpu.make_async_remote_copy(
                    src_ref=pieces.at[0, half], dst_ref=fin.at[source, o, half],
                    send_sem=fsend.at[0, half], recv_sem=frecv.at[source, o, half],
                    device_id=(sp, peers[k]), device_id_type=MESH,
                ).wait_recv()
    piece = fin.shape[4]
    for o in range(per):
        for half in range(2):
            start = (2 * o + half) * piece
            total = own_stream[:, start:start + piece]
            mixed = fin[0, o, half].astype(F32)
            for t in range(1, n_tp):
                mixed = mixed + fin[t, o, half].astype(F32)
            out_ref[:, start:start + piece] = (total + mixed).astype(BF16)

    def drain(i, carry):
        for c in range(CHUNKS):
            for half in range(2):
                d_copy(i, half, c, True).wait_send()
        return carry

    lax.fori_loop(0, n - 1, drain, 0)

    def drain_pieces(i, carry):
        for half, owner in enumerate(owners(i)):

            @pl.when(owner // per != tp)
            def _():
                f_copy(i, half, owner).wait_send()

        return carry

    lax.fori_loop(0, n, drain_pieces, 0)
    for k in range(n_tp - 1):
        p_copy(k).wait_send()
        q_copy(k).wait_send()
        y_copy(k).wait_send()


def vmem():
    return pl.BlockSpec(memory_space=pltpu.VMEM)


def hbm():
    return pl.BlockSpec(memory_space=pl.ANY)


def on_device(
    n,
    n_tp,
    residual_in,
    queries_nope,
    queries_rope,
    latents,
    rope_keys,
    latent_norm_gain,
    key_up_weight,
    value_up_weight,
    w_out,
    norm_gain,
    w_up,
    w_down,
):
    rows, model = residual_in.shape
    heads = key_up_weight.shape[1] // UNROTATED_WIDTH
    value_width = value_up_weight.shape[1] // heads
    positions = lax.axis_index("sp") * rows + jnp.arange(rows, dtype=jnp.int32)
    phases = rope_phases(positions, ROPE)
    q_rot = rotate(
        queries_rope.astype(F32).reshape(rows, heads, ROPE), phases[:, None, :]
    ).astype(BF16)
    queries = jnp.concatenate(
        [
            queries_nope.reshape(rows, heads, UNROTATED_WIDTH),
            q_rot,
            jnp.zeros((rows, heads, LANES - UNROTATED_WIDTH - ROPE), BF16),
        ],
        axis=2,
    ).reshape(rows, heads * LANES)
    lat_norm = rms_scale(latents.astype(F32), latent_norm_gain).astype(BF16)
    key_rot = rotate(rope_keys.astype(F32), phases).astype(BF16)
    x = jnp.concatenate([lat_norm, key_rot], axis=1)
    wide = x.shape[1]
    x = jnp.transpose(x.reshape(n_tp, rows // n_tp, wide), (0, 2, 1))

    width = model // n_tp
    depth, units = w_up.shape
    dma = pltpu.SemaphoreType.DMA
    part, full = pl.pallas_call(
        functools.partial(
            attention_kernel, n, n_tp, heads,
            math.log2(math.e) / math.sqrt(UNROTATED_WIDTH + ROPE)),
        out_shape=(
            jax.ShapeDtypeStruct((n_tp, rows, width), BF16),
            jax.ShapeDtypeStruct((n, 2, CHUNKS, depth // 2 // CHUNKS, units), BF16),
        ),
        in_specs=[vmem()] * 5 + [hbm()],
        out_specs=(vmem(), hbm()),
        scratch_shapes=[
            pltpu.VMEM((n, n_tp, wide, rows // n_tp), BF16),
            pltpu.VMEM((heads, rows, 1), F32),
            pltpu.VMEM((heads, rows, LANES), F32),
            dma((n - 1,)), dma((n - 1,)),
            dma((n, n_tp - 1)), dma((n, n_tp - 1)),
            dma((n - 1, 2, CHUNKS)), dma((n - 1, 2, CHUNKS)), dma,
        ],
        compiler_params=pltpu.CompilerParams(
            collective_id=0, has_side_effects=True, vmem_limit_bytes=56 * 2**20),
        name="attend",
    )(
        queries, x, jnp.transpose(key_up_weight), jnp.transpose(value_up_weight),
        w_out, w_up.reshape(2, CHUNKS, depth // 2 // CHUNKS, units),
    )

    hidden_units, share = w_down.shape
    narrow = (share // 2) % LANES != 0
    if narrow:
        down_in = jnp.transpose(w_down.reshape(hidden_units, 2, share // 2), (1, 2, 0))
        half_shape = (share // 2, hidden_units)
    else:
        down_in = w_down
        half_shape = (hidden_units, share // 2)
    per = n // n_tp
    return pl.pallas_call(
        functools.partial(feed_kernel, n, n_tp, narrow),
        out_shape=jax.ShapeDtypeStruct((rows, width), BF16),
        in_specs=[vmem(), hbm(), vmem(), hbm(), hbm()],
        out_specs=vmem(),
        scratch_shapes=[
            pltpu.VMEM((rows, width), BF16),
            pltpu.VMEM((model, units), BF16),
            pltpu.VMEM((n, 2) + half_shape, BF16),
            pltpu.VMEM((n_tp - 1, rows, width), BF16),
            pltpu.VMEM((n_tp, rows, width), BF16),
            pltpu.VMEM((n_tp, 8, rows), F32),
            pltpu.VMEM((rows, width), F32),
            pltpu.VMEM((rows, units), BF16),
            pltpu.VMEM((n, 2, rows, share // 2), BF16),
            pltpu.VMEM((n_tp, per, 2, rows, share // 2), BF16),
            dma((n - 1, 2, CHUNKS)), dma((n - 1, 2, CHUNKS)),
            dma((n_tp - 1,)), dma((n_tp - 1,)),
            dma((n_tp - 1,)), dma((n_tp - 1,)),
            dma((n_tp - 1,)), dma((n_tp - 1,)),
            dma((n, 2)), dma((n_tp, per, 2)),
            dma((4,)),
        ],
        compiler_params=pltpu.CompilerParams(
            collective_id=1, has_side_effects=True, vmem_limit_bytes=60 * 2**20),
        name="feed",
    )(part, residual_in, norm_gain.reshape(n_tp, 1, width), full.reshape(model, units), down_in)


def solution(mesh):
    in_specs = (
        P("sp", None),
        P("sp", "tp"),
        P("sp", "tp"),
        P("sp", None),
        P("sp", None),
        P(),
        P(None, "tp"),
        P(None, "tp"),
        P("tp", None),
        P(),
        P("sp", "tp"),
        P("tp", "sp"),
    )
    out_specs = P("sp", "tp")
    return jax.shard_map(
        functools.partial(on_device, mesh.shape["sp"], mesh.shape["tp"]),
        mesh=mesh, in_specs=in_specs, out_specs=out_specs, check_vma=False,
    )
```

```python
import functools
import math

import jax
import jax.numpy as jnp
from jax import lax
from jax.experimental import pallas as pl
from jax.experimental.pallas import tpu as pltpu
from jax.sharding import PartitionSpec as P

UNROTATED_WIDTH = 64
ROPE = 32
LANES = 128
CHUNKS = 4

rope_base = 10000.0
epsilon = 1e-06
F32 = jnp.float32
BF16 = jnp.bfloat16
MESH = pl.DeviceIdType.MESH
NT = (((1,), (1,)), ((), ()))


def rotate(vectors, phases):
    half_width = vectors.shape[-1] // 2
    first_half = vectors[..., :half_width]
    second_half = vectors[..., half_width:]
    cosine = jnp.cos(phases)
    sine = jnp.sin(phases)
    return jnp.concatenate(
        [first_half * cosine - second_half * sine, second_half * cosine + first_half * sine],
        axis=-1,
    )


def rope_phases(positions, width):
    inverse = 1.0 / rope_base ** (jnp.arange(0, width, 2, dtype=jnp.float32) / width)
    return positions.astype(jnp.float32)[:, None] * inverse[None, :]


def rms_scale(vectors, gain_vec):
    return (
        vectors
        * lax.rsqrt(jnp.mean(vectors * vectors, axis=-1, keepdims=True) + epsilon)
        * gain_vec
    )


def ring_of(index, n):
    return index // 2 + (index % 2) * (n - 1 - 2 * (index // 2))


def index_of(place, n):
    return 2 * place + (place // (n // 2)) * (2 * n - 1 - 4 * place)


def ring_ids(n):
    place = ring_of(lax.axis_index("sp"), n)

    def at(offset):
        return index_of((place + offset + 2 * n) % n, n)

    return at


def attention_kernel(
    n, n_tp, heads, scale, q_ref, x_ref, wk_in, wv_in, wo_ref, wu_ref,
    part_ref, full_ref,
    wk_ref, wv_ref, xs, peak, acc, xsend, xrecv, ssend, srecv, wsend, wrecv, own_sem,
):
    at = ring_ids(n)
    tp = lax.axis_index("tp")
    me = lax.axis_index("sp")
    to = ((at(1), tp), (at(-1), tp))
    peers = [(tp + k) % n_tp for k in range(1, n_tp)]
    onward = (at(1 - 2 * (tp % 2)), tp)
    barrier = pltpu.get_barrier_semaphore()
    for target in list(to) + [(me, p) for p in peers]:
        pl.semaphore_signal(barrier, inc=1, device_id=target, device_id_type=MESH)
    pl.semaphore_wait(barrier, 2 + n_tp - 1)

    latent = wk_ref.shape[1]
    value_width = wv_ref.shape[0] // heads

    def x_copy(step, src):
        return pltpu.make_async_remote_copy(
            src_ref=src, dst_ref=xs.at[step + 1, tp],
            send_sem=xsend.at[step], recv_sem=xrecv.at[step],
            device_id=onward, device_id_type=MESH,
        )

    def share(step, k):
        return pltpu.make_async_remote_copy(
            src_ref=xs.at[step, tp], dst_ref=xs.at[step, tp],
            send_sem=ssend.at[step, k], recv_sem=srecv.at[step, k],
            device_id=(me, peers[k]), device_id_type=MESH,
        )

    def share_wait(step):
        for k in range(n_tp - 1):
            pltpu.make_async_remote_copy(
                src_ref=xs.at[step, tp], dst_ref=xs.at[step, (tp + n_tp - 1 - k) % n_tp],
                send_sem=ssend.at[step, k], recv_sem=srecv.at[step, k],
                device_id=(me, peers[k]), device_id_type=MESH,
            ).wait_recv()

    def w_copy(step, half, c, first):
        owner = at(-step) if half == 0 else at(step)
        return pltpu.make_async_remote_copy(
            src_ref=wu_ref.at[half, c] if first else full_ref.at[owner, half, c],
            dst_ref=full_ref.at[owner, half, c],
            send_sem=wsend.at[step, half, c], recv_sem=wrecv.at[step, half, c],
            device_id=to[half], device_id_type=MESH,
        )

    x_copy(0, x_ref.at[tp]).start()
    for c in range(CHUNKS):
        for half in range(2):
            w_copy(0, half, c, True).start()
    own = pltpu.make_async_copy(wu_ref, full_ref.at[me], own_sem)
    own.start()
    wk_ref[...] = jnp.transpose(wk_in[...].astype(F32)).astype(BF16)
    wv_ref[...] = jnp.transpose(wv_in[...].astype(F32)).astype(BF16)
    peak[...] = jnp.full(peak.shape, -1e30, F32)
    acc[...] = jnp.zeros(acc.shape, F32)

    def attend(blocks):
        block = jnp.concatenate(blocks, axis=1)
        lat = block[:latent]
        rot = block[latent:]
        keys = block.shape[1]
        k_all = jnp.dot(wk_ref[...], lat, preferred_element_type=F32).astype(BF16)
        v_all = jnp.dot(wv_ref[...], lat, preferred_element_type=F32).astype(BF16)
        k_pad = jnp.zeros((LANES - UNROTATED_WIDTH - rot.shape[0], keys), BF16)
        ones = jnp.ones((16, keys), BF16)
        v_pad = jnp.zeros((LANES - value_width - 16, keys), BF16)
        for h in range(heads):
            k_h = jnp.concatenate(
                [k_all[h * UNROTATED_WIDTH:(h + 1) * UNROTATED_WIDTH], rot, k_pad], axis=0)
            v_h = jnp.concatenate(
                [v_all[h * value_width:(h + 1) * value_width], ones, v_pad], axis=0)
            s = jnp.dot(q_ref[:, h * LANES:(h + 1) * LANES], k_h, preferred_element_type=F32)
            old = peak[h]
            new = jnp.maximum(old, jnp.max(s, axis=1, keepdims=True))
            p = jnp.exp2((s - new) * scale).astype(BF16)
            acc[h] = acc[h] * jnp.exp2((old - new) * scale) + lax.dot_general(
                p, v_h, NT, preferred_element_type=F32)
            peak[h] = new

    def turn(i, carry):
        x_copy(i - 1, x_ref.at[tp]).wait_recv()
        x_copy(i, xs.at[i, tp]).start()
        for k in range(n_tp - 1):
            share(i, k).start()
        for c in range(CHUNKS):
            for half in range(2):
                w_copy(i - 1, half, c, True).wait_recv()
                w_copy(i, half, c, False).start()

        @pl.when(i > 1)
        def _():
            share_wait(i - 1)
            attend([xs[i - 1, t] for t in range(n_tp)])

        return carry

    attend([x_ref[t] for t in range(n_tp)])
    lax.fori_loop(1, n - 1, turn, 0)
    x_copy(n - 2, x_ref.at[tp]).wait_recv()
    for k in range(n_tp - 1):
        share(n - 1, k).start()

    def last(i, carry):
        share_wait(i)
        attend([xs[i, t] for t in range(n_tp)])
        return carry

    lax.fori_loop(n - 2, n, last, 0)

    width = part_ref.shape[2]
    group = []
    for h in range(heads):
        a = acc[h]
        group.append((a[:, :value_width] / a[:, value_width:value_width + 1]).astype(BF16))
    attended = jnp.concatenate(group, axis=1)
    for j in range(part_ref.shape[0]):
        part_ref[j] = jnp.dot(
            attended, wo_ref[:, j * width:(j + 1) * width], preferred_element_type=F32
        ).astype(BF16)

    own.wait()
    for c in range(CHUNKS):
        for half in range(2):
            w_copy(n - 2, half, c, True).wait_recv()

    def drain(i, carry):
        x_copy(i, x_ref.at[tp]).wait_send()
        for k in range(n_tp - 1):
            share(i + 1, k).wait_send()
        for c in range(CHUNKS):
            for half in range(2):
                w_copy(i, half, c, True).wait_send()
        return carry

    lax.fori_loop(0, n - 1, drain, 0)


def feed_kernel(
    n, n_tp, narrow, part_ref, res_hbm, gain_ref, up_hbm, wd_hbm,
    out_ref,
    res_ref, up, down, parts, ys, sq, own_stream, hidden, pieces, fin,
    dsend, drecv, psend, precv, ysend, yrecv, qsend, qrecv, fsend, frecv, local,
):
    at = ring_ids(n)
    tp = lax.axis_index("tp")
    sp = lax.axis_index("sp")
    to = ((at(1), tp), (at(-1), tp))
    peers = [(tp + k) % n_tp for k in range(1, n_tp)]
    barrier = pltpu.get_barrier_semaphore()
    for target in list(to) + [(sp, p) for p in peers]:
        pl.semaphore_signal(barrier, inc=1, device_id=target, device_id_type=MESH)
    pl.semaphore_wait(barrier, 2 + n_tp - 1)

    rows, width = res_ref.shape
    per = n // n_tp

    lines = down.shape[2] // CHUNKS

    def own_half(half):
        if narrow:
            return wd_hbm.at[half]
        return wd_hbm.at[:, half * down.shape[3]:(half + 1) * down.shape[3]]

    def d_copy(step, half, c, first):
        span = pl.ds(c * lines, lines)
        if not first:
            src = down.at[step, half, span]
        elif narrow:
            src = wd_hbm.at[half, span]
        else:
            src = wd_hbm.at[span, half * down.shape[3]:(half + 1) * down.shape[3]]
        return pltpu.make_async_remote_copy(
            src_ref=src, dst_ref=down.at[step + 1, half, span],
            send_sem=dsend.at[step, half, c], recv_sem=drecv.at[step, half, c],
            device_id=to[half], device_id_type=MESH,
        )

    def p_copy(k):
        peer = peers[k]
        return pltpu.make_async_remote_copy(
            src_ref=part_ref.at[peer], dst_ref=parts.at[k],
            send_sem=psend.at[k], recv_sem=precv.at[k],
            device_id=(sp, peer), device_id_type=MESH,
        )

    def y_copy(k):
        return pltpu.make_async_remote_copy(
            src_ref=ys.at[tp], dst_ref=ys.at[tp],
            send_sem=ysend.at[k], recv_sem=yrecv.at[k],
            device_id=(sp, peers[k]), device_id_type=MESH,
        )

    def q_copy(k):
        return pltpu.make_async_remote_copy(
            src_ref=sq.at[0], dst_ref=sq.at[k + 1],
            send_sem=qsend.at[k], recv_sem=qrecv.at[k],
            device_id=(sp, peers[k]), device_id_type=MESH,
        )

    def landed(step, c):
        for half in range(2):
            d_copy(step, half, c, True).wait_recv()

    def event(step, c):
        landed(step - 1, c)
        for half in range(2):
            d_copy(step, half, c, False).start()

    def events(first, last):
        for tick in range(first, last):
            event(1 + tick // CHUNKS, tick % CHUNKS)

    for c in range(CHUNKS):
        for half in range(2):
            d_copy(0, half, c, True).start()
    for k in range(n_tp - 1):
        p_copy(k).start()
    loads = [
        pltpu.make_async_copy(
            res_hbm.at[:, pl.ds(pl.multiple_of(tp * width, LANES), width)], res_ref, local.at[0]),
        pltpu.make_async_copy(up_hbm, up, local.at[1]),
        pltpu.make_async_copy(own_half(0), down.at[0, 0], local.at[2]),
        pltpu.make_async_copy(own_half(1), down.at[0, 1], local.at[3]),
    ]
    for load in loads:
        load.start()

    early = 4
    events(0, 6)
    for k in range(n_tp - 1):
        p_copy(k).wait_recv()
    loads[0].wait()
    stream = part_ref[tp].astype(F32)
    for k in range(n_tp - 1):
        stream = stream + parts[k].astype(F32)
    stream = stream + res_ref[...].astype(F32)
    own_stream[...] = stream
    ys[tp] = (stream * gain_ref[tp]).astype(BF16)
    total = jnp.sum(stream * stream, axis=1, keepdims=True)
    sq[0] = jnp.transpose(jnp.broadcast_to(total, (rows, LANES)))[:8]
    for k in range(n_tp - 1):
        q_copy(k).start()
        y_copy(k).start()
    events(6, 12)
    for k in range(n_tp - 1):
        q_copy(k).wait_recv()
    for k in range(n_tp - 1):
        pltpu.make_async_remote_copy(
            src_ref=ys.at[tp], dst_ref=ys.at[(tp + n_tp - 1 - k) % n_tp],
            send_sem=ysend.at[k], recv_sem=yrecv.at[k],
            device_id=(sp, peers[k]), device_id_type=MESH,
        ).wait_recv()
    squares = sq[0]
    for k in range(1, n_tp):
        squares = squares + sq[k]
    squares = jnp.concatenate([squares] * (LANES // 8), axis=0)
    factor = lax.rsqrt(jnp.transpose(squares)[:, :1] / (width * n_tp) + epsilon)
    loads[1].wait()
    units = hidden.shape[1]
    tile = math.gcd(units, 512)

    def up_step(c, carry):
        columns = pl.ds(pl.multiple_of(c * tile, tile), tile)
        total = jnp.dot(ys[0], up[:width, columns], preferred_element_type=F32)
        for t in range(1, n_tp):
            total = total + jnp.dot(
                ys[t], up[t * width:(t + 1) * width, columns], preferred_element_type=F32)
        total = jnp.maximum(total, 0.0) * factor
        hidden[:, columns] = (total * total).astype(BF16)

        @pl.when(c < CHUNKS)
        def _():
            event(early, c)

        return carry

    lax.fori_loop(0, units // tile, up_step, 0)

    def owners(i):
        return at(-i), at(i)

    def f_copy(i, half, owner):
        return pltpu.make_async_remote_copy(
            src_ref=pieces.at[i, half],
            dst_ref=fin.at[tp, owner % per, half],
            send_sem=fsend.at[i, half], recv_sem=frecv.at[tp, owner % per, half],
            device_id=(sp, owner // per), device_id_type=MESH,
        )

    def down_block(i, left, right):
        if narrow:
            block = jnp.concatenate([left, right], axis=0)
            half_width = left.shape[0]
            term = lax.dot_general(hidden[...], block, NT, preferred_element_type=F32)
        else:
            block = jnp.concatenate([left, right], axis=1)
            half_width = left.shape[1]
            term = jnp.dot(hidden[...], block, preferred_element_type=F32)
        term = term.astype(BF16)
        pieces[i, 0] = term[:, :half_width]
        pieces[i, 1] = term[:, half_width:]
        for half, owner in enumerate(owners(i)):

            @pl.when(owner // per != tp)
            def _():
                f_copy(i, half, owner).start()

            @pl.when(owner // per == tp)
            def _():
                fin[tp, owner % per, half] = pieces[i, half]

    for load in loads[2:]:
        load.wait()
    down_block(0, down[0, 0], down[0, 1])

    def down_step(i, carry):
        @pl.when(i <= CHUNKS)
        def _():
            event(early + 1, i - 1)

        @pl.when(i > early + 1)
        def _():
            for c in range(CHUNKS):
                landed(i - 1, c)

                @pl.when(i < n - 1)
                def _():
                    for half in range(2):
                        d_copy(i, half, c, False).start()

        down_block(i, down[i, 0], down[i, 1])
        return carry

    lax.fori_loop(1, n, down_step, 0)

    for k in range(n_tp - 1):
        source = (tp + n_tp - 1 - k) % n_tp
        for o in range(per):
            for half in range(2):
                pltpu.make_async_remote_copy(
                    src_ref=pieces.at[0, half], dst_ref=fin.at[source, o, half],
                    send_sem=fsend.at[0, half], recv_sem=frecv.at[source, o, half],
                    device_id=(sp, peers[k]), device_id_type=MESH,
                ).wait_recv()
    piece = fin.shape[4]
    for o in range(per):
        for half in range(2):
            start = (2 * o + half) * piece
            total = own_stream[:, start:start + piece]
            mixed = fin[0, o, half].astype(F32)
            for t in range(1, n_tp):
                mixed = mixed + fin[t, o, half].astype(F32)
            out_ref[:, start:start + piece] = (total + mixed).astype(BF16)

    def drain(i, carry):
        for c in range(CHUNKS):
            for half in range(2):
                d_copy(i, half, c, True).wait_send()
        return carry

    lax.fori_loop(0, n - 1, drain, 0)

    def drain_pieces(i, carry):
        for half, owner in enumerate(owners(i)):

            @pl.when(owner // per != tp)
            def _():
                f_copy(i, half, owner).wait_send()

        return carry

    lax.fori_loop(0, n, drain_pieces, 0)
    for k in range(n_tp - 1):
        p_copy(k).wait_send()
        q_copy(k).wait_send()
        y_copy(k).wait_send()


def vmem():
    return pl.BlockSpec(memory_space=pltpu.VMEM)


def hbm():
    return pl.BlockSpec(memory_space=pl.ANY)


def on_device(
    n,
    n_tp,
    residual_in,
    queries_nope,
    queries_rope,
    latents,
    rope_keys,
    latent_norm_gain,
    key_up_weight,
    value_up_weight,
    w_out,
    norm_gain,
    w_up,
    w_down,
):
    rows, model = residual_in.shape
    heads = key_up_weight.shape[1] // UNROTATED_WIDTH
    value_width = value_up_weight.shape[1] // heads
    positions = lax.axis_index("sp") * rows + jnp.arange(rows, dtype=jnp.int32)
    phases = rope_phases(positions, ROPE)
    q_rot = rotate(
        queries_rope.astype(F32).reshape(rows, heads, ROPE), phases[:, None, :]
    ).astype(BF16)
    queries = jnp.concatenate(
        [
            queries_nope.reshape(rows, heads, UNROTATED_WIDTH),
            q_rot,
            jnp.zeros((rows, heads, LANES - UNROTATED_WIDTH - ROPE), BF16),
        ],
        axis=2,
    ).reshape(rows, heads * LANES)
    lat_norm = rms_scale(latents.astype(F32), latent_norm_gain).astype(BF16)
    key_rot = rotate(rope_keys.astype(F32), phases).astype(BF16)
    x = jnp.concatenate([lat_norm, key_rot], axis=1)
    wide = x.shape[1]
    x = jnp.transpose(x.reshape(n_tp, rows // n_tp, wide), (0, 2, 1))

    width = model // n_tp
    depth, units = w_up.shape
    dma = pltpu.SemaphoreType.DMA
    part, full = pl.pallas_call(
        functools.partial(
            attention_kernel, n, n_tp, heads,
            math.log2(math.e) / math.sqrt(UNROTATED_WIDTH + ROPE)),
        out_shape=(
            jax.ShapeDtypeStruct((n_tp, rows, width), BF16),
            jax.ShapeDtypeStruct((n, 2, CHUNKS, depth // 2 // CHUNKS, units), BF16),
        ),
        in_specs=[vmem()] * 5 + [hbm()],
        out_specs=(vmem(), hbm()),
        scratch_shapes=[
            pltpu.VMEM(key_up_weight.shape[::-1], BF16),
            pltpu.VMEM(value_up_weight.shape[::-1], BF16),
            pltpu.VMEM((n, n_tp, wide, rows // n_tp), BF16),
            pltpu.VMEM((heads, rows, 1), F32),
            pltpu.VMEM((heads, rows, LANES), F32),
            dma((n - 1,)), dma((n - 1,)),
            dma((n, n_tp - 1)), dma((n, n_tp - 1)),
            dma((n - 1, 2, CHUNKS)), dma((n - 1, 2, CHUNKS)), dma,
        ],
        compiler_params=pltpu.CompilerParams(
            collective_id=0, has_side_effects=True, vmem_limit_bytes=56 * 2**20),
        name="attend",
    )(
        queries, x, key_up_weight, value_up_weight,
        w_out, w_up.reshape(2, CHUNKS, depth // 2 // CHUNKS, units),
    )

    hidden_units, share = w_down.shape
    narrow = (share // 2) % LANES != 0
    if narrow:
        down_in = jnp.transpose(w_down.reshape(hidden_units, 2, share // 2), (1, 2, 0))
        half_shape = (share // 2, hidden_units)
    else:
        down_in = w_down
        half_shape = (hidden_units, share // 2)
    per = n // n_tp
    return pl.pallas_call(
        functools.partial(feed_kernel, n, n_tp, narrow),
        out_shape=jax.ShapeDtypeStruct((rows, width), BF16),
        in_specs=[vmem(), hbm(), vmem(), hbm(), hbm()],
        out_specs=vmem(),
        scratch_shapes=[
            pltpu.VMEM((rows, width), BF16),
            pltpu.VMEM((model, units), BF16),
            pltpu.VMEM((n, 2) + half_shape, BF16),
            pltpu.VMEM((n_tp - 1, rows, width), BF16),
            pltpu.VMEM((n_tp, rows, width), BF16),
            pltpu.VMEM((n_tp, 8, rows), F32),
            pltpu.VMEM((rows, width), F32),
            pltpu.VMEM((rows, units), BF16),
            pltpu.VMEM((n, 2, rows, share // 2), BF16),
            pltpu.VMEM((n_tp, per, 2, rows, share // 2), BF16),
            dma((n - 1, 2, CHUNKS)), dma((n - 1, 2, CHUNKS)),
            dma((n_tp - 1,)), dma((n_tp - 1,)),
            dma((n_tp - 1,)), dma((n_tp - 1,)),
            dma((n_tp - 1,)), dma((n_tp - 1,)),
            dma((n, 2)), dma((n_tp, per, 2)),
            dma((4,)),
        ],
        compiler_params=pltpu.CompilerParams(
            collective_id=1, has_side_effects=True, vmem_limit_bytes=60 * 2**20),
        name="feed",
    )(part, residual_in, norm_gain.reshape(n_tp, 1, width), full.reshape(model, units), down_in)


def solution(mesh):
    in_specs = (
        P("sp", None),
        P("sp", "tp"),
        P("sp", "tp"),
        P("sp", None),
        P("sp", None),
        P(),
        P(None, "tp"),
        P(None, "tp"),
        P("tp", None),
        P(),
        P("sp", "tp"),
        P("tp", "sp"),
    )
    out_specs = P("sp", "tp")
    return jax.shard_map(
        functools.partial(on_device, mesh.shape["sp"], mesh.shape["tp"]),
        mesh=mesh, in_specs=in_specs, out_specs=out_specs, check_vma=False,
    )
```
